32 devices in a mesh: rep: 2 (over x), fs: 4 (over y, core), tp: 4 (over z).
Axes of the slice: x: 2, y: 2, z: 4, core: 2. Of those that a mesh axis runs over, the one named last changes fastest.
Arguments:
- acts: bfloat16 [2048, 2048], P(('rep', 'fs'), 'tp'), may hold values from -6 to 6
- cotangent: bfloat16 [2048, 2048], P(('rep', 'fs'), 'tp'), may hold values from -8 to 8
- pre_act: bfloat16 [2048, 4096], P(('rep', 'fs'), 'tp'), may hold values from -6 to 6
- up_store: float32 [2048, 4096], P('fs', 'tp'), may hold values from -0.125 to 0.125
- up_scale: float32 [4096], P('tp'), may hold values from 0.5 to 2
- down_store: float32 [4096, 2048], P('tp', 'fs'), may hold values from -0.09375 to 0.09375
- down_scale: float32 [2048], replicated, may hold values from 0.5 to 2
Outputs:
- grad_input: bfloat16 [2048, 2048], P(('rep', 'fs'), 'tp')
- grad_up: float32 [2048, 4096], P('fs', 'tp')
- grad_down: float32 [4096, 2048], P('tp', 'fs')
The draws below stay inside these ranges and needn't reach their ends.
All inputs are finite; a program needn't handle non-finite values.
Results may differ from the reference program's by a relative error of at most 0.007.
Values may be sent and summed in bfloat16 or wider, within the bound.
No kernel may reach another device: no remote copies, remote signals or barrier semaphores. Data moves between devices by JAX's collectives and lax.ppermute only.
A program may use at most 128 MiB of HBM per device.

```python
import math
import jax
import jax.numpy as jnp

D = 2048
FF = 4096
TOKENS = 2048


def with_spikes(entries, rng, source, target, blocks, factor):
    owner, partner = [(jnp.arange(entries.shape[dim]) // (entries.shape[dim] // blocks)).reshape([-1 if axis == dim else 1 for axis in range(entries.ndim)]) for dim in (source, target)]
    chosen = jax.random.permutation(rng, blocks)[partner]
    strong = (owner == chosen) | (owner == (partner + blocks // 2) % blocks)
    return jnp.where(strong, factor * entries, entries)


def block_scale(own_key, shape, split, smallest, high):
    gain, own = 1.0, jax.random.fold_in(own_key, 6)
    for axis_at, parts in split:
        draws = jnp.exp(jax.random.uniform(jax.random.fold_in(own, axis_at), (parts,), jnp.float32, smallest / len(split), high / len(split)))
        gain = gain * jnp.repeat(draws, shape[axis_at] // parts).reshape([-1 if axis == axis_at else 1 for axis in range(len(shape))])
    return gain


def noise(stream_key, shape, scale, limit, pieces=(), kind=jnp.bfloat16):
    result = jax.random.normal(stream_key, shape, jnp.float32) * scale
    if len(pieces) > 0:
        result = block_scale(stream_key, shape, pieces, -0.22, 0.18) * result
    return jnp.clip(result, min=-limit, max=limit).astype(kind)


def gaussian_with(key, dims, spread, bound, cuts, heavy, dtype=jnp.bfloat16):
    array = spread * jax.random.normal(key, dims, jnp.float32)
    if cuts:
        array = array * block_scale(key, dims, cuts, -0.22, 0.18)
    return jnp.clip(with_spikes(array, jax.random.fold_in(key, 3), *heavy), -bound, bound).astype(dtype)


def setup_inputs(seed: int = 0) -> dict:
    arg_keys = jax.random.split(jax.random.key(seed), 8)
    return {
        "acts": noise(arg_keys[0], (TOKENS, D), 1.0, 6.0, ((0, 8), (1, 4))),
        "cotangent": gaussian_with(arg_keys[1], (TOKENS, D), 1.0, 8.0, ((0, 8), (1, 4)), (0, 1, 8, 2.0)),
        "pre_act": noise(arg_keys[2], (TOKENS, FF), 1.0, 6.0, ((0, 8), (1, 4))),
        "up_store": noise(arg_keys[3], (D, FF), D ** -0.5, 0.125, ((0, 4), (1, 4)), jnp.float32),
        "up_scale": jnp.clip(jnp.exp(math.log(2.0) - 1.3862944 * jax.random.uniform(arg_keys[4], (FF,), jnp.float32) ** block_scale(arg_keys[4], (FF,), ((0, 4),), -0.2, 0.2)), 0.5, 2.0),
        "down_store": noise(arg_keys[5], (FF, D), FF ** -0.5, 0.09375, ((0, 4), (1, 4)), jnp.float32),
        "down_scale": jnp.clip(jnp.exp(jax.random.uniform(arg_keys[6], (D,), jnp.float32, math.log(0.5), math.log(2.0))), 0.5, 2.0),
    }


def reference(acts, cotangent, pre_act, up_store, up_scale, down_store, down_scale):
    norm_factor = 1.0 / math.sqrt(TOKENS)
    scaled = (cotangent.astype(jnp.float32) * down_scale[None, :]).astype(jnp.bfloat16)
    d_act = jnp.dot(scaled, down_store.astype(jnp.bfloat16).T, preferred_element_type=jnp.float32)
    positive = jnp.maximum(pre_act.astype(jnp.float32), 0.0)
    act = (positive * positive).astype(jnp.bfloat16)
    d_pre = (2.0 * positive * d_act * up_scale[None, :]).astype(jnp.bfloat16)
    grad_down = jnp.dot(act.T, scaled, preferred_element_type=jnp.float32) * norm_factor
    grad_up = jnp.dot(acts.T, d_pre, preferred_element_type=jnp.float32) * norm_factor
    grad_input = jnp.dot(d_pre, up_store.astype(jnp.bfloat16).T, preferred_element_type=jnp.float32).astype(jnp.bfloat16)
    return (grad_input, grad_up, grad_down)
```

```python
import math

import jax
import jax.numpy as jnp
from jax import lax
from jax.sharding import PartitionSpec as P


BOTH = ("fs", "tp")


def contract_last(left, right):
    return lax.dot_general(
        left, right, (((1,), (1,)), ((), ())), preferred_element_type=jnp.float32
    )


def contract_first(left, right):
    return lax.dot_general(
        left, right, (((0,), (0,)), ((), ())), preferred_element_type=jnp.float32
    )


def round_bf16(x):
    return lax.reduce_precision(x, exponent_bits=8, mantissa_bits=7)


def rep_sum(x):
    if lax.axis_size("rep") != 2:
        return lax.psum(x, "rep")
    own = round_bf16(x)
    other = lax.ppermute(own.astype(jnp.bfloat16), "rep", [(0, 1), (1, 0)])
    return own + other.astype(jnp.float32)


def body(acts, cotangent, pre_act, up_store, up_scale, down_store, down_scale):
    nf, nt = lax.axis_size("fs"), lax.axis_size("tp")
    per = nf // nt
    f, t = lax.axis_index("fs"), lax.axis_index("tp")
    tok, cols = acts.shape
    width = up_store.shape[0]
    norm_factor = 1.0 / math.sqrt(tok * nf * lax.axis_size("rep"))
    slots = [(s, a) for s in range(nt) for a in range(per)]

    def token_block(fi, ti, s, a):
        return (fi + (ti - s) * per + a) % nf

    def grid(target):
        return [
            (fi * nt + ti, target(fi, ti)) for fi in range(nf) for ti in range(nt)
        ]

    def to_owner(s, a):
        return grid(lambda fi, ti: token_block(fi, ti, s, a) * nt + ti)

    def from_owner(s, a):
        return [(dst, src) for src, dst in to_owner(s, a)]

    def home(a):
        return grid(lambda fi, ti: token_block(fi, ti, 0, a) * nt + fi // per)

    def away(a):
        return [(dst, src) for src, dst in home(a)]

    def part_at(a):
        return ((f - a) % per) * width

    def to_features(x):
        base = []
        for a in range(per):
            piece = x if per == 1 else lax.dynamic_slice_in_dim(x, part_at(a), width, 1)
            base.append(lax.ppermute(piece, BOTH, away(a)))
        return [
            base[a]
            if s == 0
            else lax.ppermute(base[a], "tp", [(i, (i + s) % nt) for i in range(nt)])
            for s, a in slots
        ]

    scale_here = lax.dynamic_slice_in_dim(down_scale, t * cols, cols, 0)
    scaled = (cotangent.astype(jnp.float32) * scale_here[None, :]).astype(jnp.bfloat16)
    scaled_blocks = to_features(scaled)
    positive = jnp.maximum(pre_act.astype(jnp.float32), 0.0)
    act = (positive * positive).astype(jnp.bfloat16)
    down_bf = down_store.astype(jnp.bfloat16)
    up_bf = up_store.astype(jnp.bfloat16)

    d_act = 0.0
    for (s, a), block in zip(slots, scaled_blocks):
        partial_value = contract_last(block, down_bf).astype(jnp.bfloat16)
        d_act += lax.ppermute(partial_value, BOTH, to_owner(s, a)).astype(jnp.float32)
    d_pre = (2.0 * positive * d_act * up_scale[None, :]).astype(jnp.bfloat16)

    act_blocks = [lax.ppermute(act, BOTH, from_owner(s, a)) for s, a in slots]
    acts_blocks = to_features(acts)
    grad_down = rep_sum(
        contract_first(jnp.concatenate(act_blocks), jnp.concatenate(scaled_blocks)) * norm_factor
    )

    dpre_blocks = [lax.ppermute(d_pre, BOTH, from_owner(s, a)) for s, a in slots]
    sums = [0.0] * per
    for (s, a), block in zip(slots, dpre_blocks):
        value = contract_last(block, up_bf)
        if s:
            value = lax.ppermute(
                value.astype(jnp.bfloat16), "tp", [(i, (i - s) % nt) for i in range(nt)]
            ).astype(jnp.float32)
        sums[a] += value
    pieces = [
        lax.ppermute(sums[a].astype(jnp.bfloat16), BOTH, home(a)) for a in range(per)
    ]
    if per == 1:
        grad_input = pieces[0]
    else:
        grad_input = jnp.zeros((tok, cols), jnp.bfloat16)
        for a in range(per):
            grad_input = lax.dynamic_update_slice_in_dim(grad_input, pieces[a], part_at(a), 1)

    grad_up = rep_sum(
        contract_first(jnp.concatenate(acts_blocks), jnp.concatenate(dpre_blocks)) * norm_factor
    )
    return (grad_input, grad_up, grad_down)


def solution(mesh):
    return jax.shard_map(
        body,
        mesh=mesh,
        in_specs=(
            P(("rep", "fs"), "tp"),
            P(("rep", "fs"), "tp"),
            P(("rep", "fs"), "tp"),
            P("fs", "tp"),
            P("tp"),
            P("tp", "fs"),
            P(),
        ),
        out_specs=(P(("rep", "fs"), "tp"), P("fs", "tp"), P("tp", "fs")),
        check_vma=False,
    )
```

```python
import math

import jax
import jax.numpy as jnp
from jax import lax
from jax.sharding import PartitionSpec as P


BOTH = ("fs", "tp")


def contract_last(left, right):
    return lax.dot_general(
        left, right, (((1,), (1,)), ((), ())), preferred_element_type=jnp.float32
    )


def contract_first(left, right):
    return lax.dot_general(
        left, right, (((0,), (0,)), ((), ())), preferred_element_type=jnp.float32
    )


def round_bf16(x):
    return lax.reduce_precision(x, exponent_bits=8, mantissa_bits=7)


def rep_sum(x):
    if lax.axis_size("rep") != 2:
        return lax.psum(x, "rep")
    own = round_bf16(x)
    other = lax.ppermute(own.astype(jnp.bfloat16), "rep", [(0, 1), (1, 0)])
    return own + other.astype(jnp.float32)


def body(acts, cotangent, pre_act, up_store, up_scale, down_store, down_scale):
    nf, nt = lax.axis_size("fs"), lax.axis_size("tp")
    per = nf // nt
    f, t = lax.axis_index("fs"), lax.axis_index("tp")
    tok, cols = acts.shape
    width = up_store.shape[0]
    norm_factor = 1.0 / math.sqrt(tok * nf * lax.axis_size("rep"))
    slots = [(s, a) for s in range(nt) for a in range(per)]

    def token_block(fi, ti, s, a):
        return (fi + (ti - s) * per + a) % nf

    def grid(target):
        return [
            (fi * nt + ti, target(fi, ti)) for fi in range(nf) for ti in range(nt)
        ]

    def to_owner(s, a):
        return grid(lambda fi, ti: token_block(fi, ti, s, a) * nt + ti)

    def from_owner(s, a):
        return [(dst, src) for src, dst in to_owner(s, a)]

    def home(a):
        return grid(lambda fi, ti: token_block(fi, ti, 0, a) * nt + fi // per)

    def away(a):
        return [(dst, src) for src, dst in home(a)]

    def part_at(a):
        return ((f - a) % per) * width

    def to_features(x):
        base = []
        for a in range(per):
            piece = x if per == 1 else lax.dynamic_slice_in_dim(x, part_at(a), width, 1)
            base.append(lax.ppermute(piece, BOTH, away(a)))
        return [
            base[a]
            if s == 0
            else lax.ppermute(base[a], "tp", [(i, (i + s) % nt) for i in range(nt)])
            for s, a in slots
        ]

    scale_here = lax.dynamic_slice_in_dim(down_scale, t * cols, cols, 0)
    scaled = (cotangent.astype(jnp.float32) * scale_here[None, :]).astype(jnp.bfloat16)
    scaled_blocks = to_features(scaled)
    positive = jnp.maximum(pre_act.astype(jnp.float32), 0.0)
    act = (positive * positive).astype(jnp.bfloat16)
    down_bf = down_store.astype(jnp.bfloat16)
    up_bf = up_store.astype(jnp.bfloat16)

    d_act = 0.0
    for (s, a), block in zip(slots, scaled_blocks):
        partial_value = contract_last(block, down_bf).astype(jnp.bfloat16)
        d_act += lax.ppermute(partial_value, BOTH, to_owner(s, a)).astype(jnp.float32)
    late_pre, d_act = lax.optimization_barrier((pre_act, d_act))
    positive = jnp.maximum(late_pre.astype(jnp.float32), 0.0)
    d_pre = (2.0 * positive * d_act * up_scale[None, :]).astype(jnp.bfloat16)

    act_blocks = [lax.ppermute(act, BOTH, from_owner(s, a)) for s, a in slots]
    acts_blocks = to_features(acts)
    grad_down = rep_sum(
        contract_first(jnp.concatenate(act_blocks), jnp.concatenate(scaled_blocks)) * norm_factor
    )

    dpre_blocks = [lax.ppermute(d_pre, BOTH, from_owner(s, a)) for s, a in slots]
    sums = [0.0] * per
    for (s, a), block in zip(slots, dpre_blocks):
        value = contract_last(block, up_bf)
        if s:
            value = lax.ppermute(
                value.astype(jnp.bfloat16), "tp", [(i, (i - s) % nt) for i in range(nt)]
            ).astype(jnp.float32)
        sums[a] += value
    pieces = [lax.ppermute(sums[a].astype(jnp.bfloat16), BOTH, home(a)) for a in range(per)]
    if per == 1:
        grad_input = pieces[0]
    else:
        grad_input = jnp.zeros((tok, cols), jnp.bfloat16)
        for a in range(per):
            grad_input = lax.dynamic_update_slice_in_dim(grad_input, pieces[a], part_at(a), 1)

    grad_up = rep_sum(
        contract_first(jnp.concatenate(acts_blocks), jnp.concatenate(dpre_blocks)) * norm_factor
    )
    return (grad_input, grad_up, grad_down)


def solution(mesh):
    return jax.shard_map(
        body,
        mesh=mesh,
        in_specs=(
            P(("rep", "fs"), "tp"),
            P(("rep", "fs"), "tp"),
            P(("rep", "fs"), "tp"),
            P("fs", "tp"),
            P("tp"),
            P("tp", "fs"),
            P(),
        ),
        out_specs=(P(("rep", "fs"), "tp"), P("fs", "tp"), P("tp", "fs")),
        check_vma=False,
    )
```

```python
import math

import jax
import jax.numpy as jnp
from jax import lax
from jax.sharding import PartitionSpec as P


BOTH = ("fs", "tp")


def contract_last(left, right):
    return lax.dot_general(
        left, right, (((1,), (1,)), ((), ())), preferred_element_type=jnp.float32
    )


def contract_first(left, right):
    return lax.dot_general(
        left, right, (((0,), (0,)), ((), ())), preferred_element_type=jnp.float32
    )


def round_bf16(x):
    return lax.reduce_precision(x, exponent_bits=8, mantissa_bits=7)


def move(x, axis, pairs):
    return lax.ppermute(x, axis, pairs)


def rep_sum(x):
    if lax.axis_size("rep") != 2:
        return lax.psum(x, "rep")
    own = round_bf16(x)
    other = move(own.astype(jnp.bfloat16), "rep", [(0, 1), (1, 0)])
    return own + other.astype(jnp.float32)


def body(acts, cotangent, pre_act, up_store, up_scale, down_store, down_scale):
    nf, nt = lax.axis_size("fs"), lax.axis_size("tp")
    per = nf // nt
    f, t = lax.axis_index("fs"), lax.axis_index("tp")
    tok, cols = acts.shape
    width = up_store.shape[0]
    norm_factor = 1.0 / math.sqrt(tok * nf * lax.axis_size("rep"))
    slots = [(s, a) for s in range(nt) for a in range(per)]

    def token_block(fi, ti, s, a):
        return fi ^ ((ti ^ s) * per + a)

    def grid(target):
        return [
            (fi * nt + ti, target(fi, ti)) for fi in range(nf) for ti in range(nt)
        ]

    def to_owner(s, a):
        return grid(lambda fi, ti: token_block(fi, ti, s, a) * nt + ti)

    def all_tokens(x):
        blocks = [x]
        for i in range(1, nf):
            source, step = (blocks[i - 1], 1) if i % 2 else (x, i)
            blocks.append(move(source, "fs", [(j, j ^ step) for j in range(nf)]))
        return jnp.concatenate(blocks)

    def by_place(blocks):
        stack = jnp.concatenate(blocks)
        rows = per * tok
        return jnp.concatenate(
            [lax.dynamic_slice_in_dim(stack, (t ^ s) * rows, rows, 0) for s in range(nt)]
        )

    def home(a):
        return grid(lambda fi, ti: token_block(fi, ti, 0, a) * nt + fi // per)

    def away(a):
        return [(dst, src) for src, dst in home(a)]

    def part_at(a):
        return ((f % per) ^ a) * width

    def to_features(x):
        base = []
        for a in range(per):
            piece = x if per == 1 else lax.dynamic_slice_in_dim(x, part_at(a), width, 1)
            base.append(move(piece, BOTH, away(a)))
        return [
            base[a]
            if s == 0
            else move(base[a], "tp", [(i, i ^ s) for i in range(nt)])
            for s, a in slots
        ]

    scale_here = lax.dynamic_slice_in_dim(down_scale, t * cols, cols, 0)
    scaled = (cotangent.astype(jnp.float32) * scale_here[None, :]).astype(jnp.bfloat16)
    scaled_blocks = to_features(scaled)
    positive = jnp.maximum(pre_act.astype(jnp.float32), 0.0)
    act = (positive * positive).astype(jnp.bfloat16)
    down_bf = down_store.astype(jnp.bfloat16)
    up_bf = up_store.astype(jnp.bfloat16)

    d_act = 0.0
    for (s, a), block in zip(slots, scaled_blocks):
        partial_value = contract_last(block, down_bf).astype(jnp.bfloat16)
        d_act += move(partial_value, BOTH, to_owner(s, a)).astype(jnp.float32)
    late_pre, d_act = lax.optimization_barrier((pre_act, d_act))
    positive = jnp.maximum(late_pre.astype(jnp.float32), 0.0)
    d_pre = (2.0 * positive * d_act * up_scale[None, :]).astype(jnp.bfloat16)

    act_all = all_tokens(act)
    acts_blocks = to_features(acts)
    scaled_all = by_place(scaled_blocks)
    down_part = contract_first(act_all, scaled_all) * norm_factor
    grad_down = rep_sum(down_part)

    dpre_all = all_tokens(d_pre)
    sums = [0.0] * per
    for s, a in slots:
        block = lax.dynamic_slice_in_dim(dpre_all, ((t ^ s) * per + a) * tok, tok, 0)
        value = contract_last(block, up_bf)
        if s:
            value = move(
                value.astype(jnp.bfloat16), "tp", [(i, i ^ s) for i in range(nt)]
            ).astype(jnp.float32)
        sums[a] += value
    pieces = [move(sums[a].astype(jnp.bfloat16), BOTH, home(a)) for a in range(per)]
    if per == 1:
        grad_input = pieces[0]
    else:
        grad_input = jnp.zeros((tok, cols), jnp.bfloat16)
        for a in range(per):
            grad_input = lax.dynamic_update_slice_in_dim(grad_input, pieces[a], part_at(a), 1)

    grad_up = rep_sum(contract_first(by_place(acts_blocks), dpre_all) * norm_factor)
    return (grad_input, grad_up, grad_down)


def solution(mesh):
    return jax.shard_map(
        body,
        mesh=mesh,
        in_specs=(
            P(("rep", "fs"), "tp"),
            P(("rep", "fs"), "tp"),
            P(("rep", "fs"), "tp"),
            P("fs", "tp"),
            P("tp"),
            P("tp", "fs"),
            P(),
        ),
        out_specs=(P(("rep", "fs"), "tp"), P("fs", "tp"), P("tp", "fs")),
        check_vma=False,
    )
```
